32 devices in a mesh: row: 8 (over z, core), col: 4 (over y, x).
Axes of the slice: x: 2, y: 2, z: 4, core: 2. Of those that a mesh axis runs over, the one named last changes fastest.
Arguments:
- tokens: bfloat16 [4096, 2048], P('row'), may hold values from -6 to 6
- out_weight: bfloat16 [2048, 2048], P(None, 'col'), may hold values from -0.125 to 0.125
Outputs:
- mixed: bfloat16 [4096, 2048], P('row', 'col')
The draws below stay inside these ranges and needn't reach their ends.
All inputs are finite; a program needn't handle non-finite values.
Results may differ from the reference program's by a relative error of at most 0.001.
Values may be sent and summed in bfloat16 or wider, within the bound.
A program may use at most 64 MiB of HBM per device.

```python
import jax
import jax.numpy as jnp
from jax import lax

D = 2048
GROUPS = 4
GROUP_DIM = 512
LENGTH = 4096


def levels(own_key, extent, split, smallest, largest):
    def one(axis_at, parts):
        draws = jax.random.uniform(jax.random.fold_in(jax.random.fold_in(own_key, 6), axis_at), (parts,), jnp.float32, smallest / len(split), largest / len(split))
        return jnp.repeat(jnp.exp(draws), extent[axis_at] // parts).reshape((-1,) + (1,) * (len(extent) - axis_at - 1))

    factor_of = one(*split[0])
    for cut in split[1:]:
        factor_of = factor_of * one(*cut)
    return factor_of


def noise(rng, extent, width, bound, cuts=(), dtype=jnp.bfloat16):
    drawn = width * jax.random.normal(rng, extent, jnp.float32)
    if cuts:
        drawn = drawn * levels(rng, extent, cuts, -0.22, 0.18)
    return jnp.clip(drawn, -bound, bound).astype(dtype)


def setup_inputs(seed: int = 0) -> dict:
    keys = jax.random.split(jax.random.key(seed), 3)
    tokens = noise(keys[0], (LENGTH, D), 1.0, 6.0, ((0, 8),))
    out_weight = noise(keys[1], (D, D), D ** -0.5, 0.125, ((1, 4),))
    return {"tokens": tokens, "out_weight": out_weight}


def per_group(block):
    return jnp.fft.fft2(block, norm="ortho").real.astype(jnp.float32)


def reference(tokens, out_weight):
    grouped = tokens.astype(jnp.float32).reshape(LENGTH, GROUPS, GROUP_DIM)
    spectra = lax.map(per_group, jnp.moveaxis(grouped, 1, 0))
    spectral = jnp.moveaxis(spectra, 0, 1).reshape(LENGTH, D).astype(jnp.float32)
    mixed = jnp.dot(spectral, out_weight.astype(jnp.float32), precision=lax.Precision.HIGHEST, preferred_element_type=jnp.float32)
    return mixed.astype(jnp.bfloat16)
```

```python
import math

import functools

import jax
import jax.numpy as jnp
import numpy as np
from jax import lax
from jax.experimental import pallas as pl
from jax.experimental.pallas import tpu as pltpu
from jax.sharding import PartitionSpec as P

GROUPS = 4
GROUP_DIM = 512


def angles(product, period):
    return (product % period).astype(jnp.float32) * (2.0 * math.pi / period)


def plain_dot(matrix, values):
    return jnp.dot(
        matrix, values, precision=lax.Precision.HIGHEST, preferred_element_type=jnp.float32
    )


def whole_transform(whole_rows, row_count, seg_rows, length):
    few_chans = whole_rows.shape[2]
    lattice = jnp.arange(row_count, dtype=jnp.int32)
    phases = angles(lattice[:, None] * lattice[None, :], row_count)
    cosine_table = jnp.cos(phases)
    sine_table = jnp.sin(phases)
    real_in = whole_rows[0].reshape(row_count, seg_rows * few_chans)
    imag_in = whole_rows[1].reshape(row_count, seg_rows * few_chans)
    first_re = (plain_dot(cosine_table, real_in) + plain_dot(sine_table, imag_in)).reshape(
        row_count, seg_rows, few_chans
    )
    first_im = (plain_dot(cosine_table, imag_in) - plain_dot(sine_table, real_in)).reshape(
        row_count, seg_rows, few_chans
    )
    inner = jnp.arange(seg_rows, dtype=jnp.int32)
    twist = angles(lattice[:, None] * inner[None, :], length)[:, :, None]
    twist_cos = jnp.cos(twist)
    twist_sin = jnp.sin(twist)
    turned_re = twist_cos * first_re + twist_sin * first_im
    turned_im = twist_cos * first_im - twist_sin * first_re
    folded_re = jnp.transpose(turned_re, (1, 0, 2)).reshape(seg_rows, row_count * few_chans)
    folded_im = jnp.transpose(turned_im, (1, 0, 2)).reshape(seg_rows, row_count * few_chans)
    seg_phases = angles(inner[:, None] * inner[None, :], seg_rows)
    real_part = plain_dot(jnp.cos(seg_phases), folded_re) + plain_dot(
        jnp.sin(seg_phases), folded_im
    )
    return real_part.reshape(length, few_chans)


def general_body(tokens, out_weight):
    seg_rows = tokens.shape[0]
    col_width = out_weight.shape[1]
    row_count = lax.axis_size("row")
    length = seg_rows * row_count
    scaling = 1.0 / math.sqrt(length * GROUP_DIM)
    weight_wide = out_weight.astype(jnp.float32)
    lattice = jnp.arange(GROUP_DIM, dtype=jnp.int32)
    phases = angles(lattice[:, None] * lattice[None, :], GROUP_DIM)
    cosine_table = jnp.cos(phases) * scaling
    sine_table = jnp.sin(phases) * scaling
    folded_rows = []
    for group in range(GROUPS):
        group_rows = weight_wide[group * GROUP_DIM : (group + 1) * GROUP_DIM]
        folded_rows.append(
            jnp.concatenate(
                [plain_dot(cosine_table, group_rows), -plain_dot(sine_table, group_rows)], axis=1
            )
        )
    folded_map = jnp.concatenate(folded_rows, axis=0)
    spectrum = plain_dot(tokens.astype(jnp.float32), folded_map)
    stacked = jnp.stack([spectrum[:, :col_width], spectrum[:, col_width:]])
    whole_rows = lax.all_to_all(stacked, "row", split_axis=2, concat_axis=1, tiled=True)
    ordered = whole_transform(whole_rows, row_count, seg_rows, length)
    spectral = lax.all_to_all(
        ordered.astype(jnp.bfloat16), "row", split_axis=0, concat_axis=1, tiled=True
    )
    return spectral

RADIX = 8
HALF = 64
QUARTER = 32
LANES = 128
EXTRA = 16
ROWS = 8
COLS = 4
SLOTS = 8
CODE = 84.0
LATE = 4
TALL = 32
UNROLL = 2
MESH = pl.DeviceIdType.MESH


def split_table(values):
    big = values.astype(jnp.bfloat16)
    return big, (values - big.astype(np.float64)).astype(jnp.bfloat16)


def tables(size, length):
    index = np.arange(size)
    phase = 2.0 * np.pi * ((index[:, None] * index[None, :]) % size) / size
    high, low = split_table(np.concatenate([np.cos(phase), np.sin(phase)], axis=0))
    turn = 2.0 * np.pi * (index[:, None] * np.arange(RADIX)[None, :]) / length
    twist = np.zeros((size, LANES), np.float32)
    twist[:, :RADIX] = np.cos(turn)
    twist[:, RADIX : 2 * RADIX] = np.sin(turn)
    return high, low, twist


def dot(a, b):
    return jnp.dot(a, b, preferred_element_type=jnp.float32)


def split(values):
    high = values.astype(jnp.bfloat16)
    return high, (values - high.astype(jnp.float32)).astype(jnp.bfloat16)


def row_of(slot, upper):
    return ROWS // 4 + upper * (ROWS // 4) + slot % 2


def kernel(
    scaling,
    tok_hbm,
    w_hbm,
    high_hbm,
    low_hbm,
    twist_ref,
    out_ref,
    tok_ref,
    w_ref,
    high_ref,
    low_ref,
    tok_s,
    tok_r,
    turn_c,
    turn_s,
    found,
    packed,
    code_s,
    gathered,
    fold_high,
    fold_low,
    total,
    load_sem,
    tok_send,
    tok_recv,
    code_send,
    code_recv,
    side_send,
    side_recv,
):
    me = lax.axis_index("row")
    col = lax.axis_index("col")
    size = tok_ref.shape[0]
    inner = size // RADIX
    mid = size // 2
    groups = w_ref.shape[0] // size
    upper = me // (ROWS // 2)
    central = jnp.logical_and(me >= ROWS // 4, me < 3 * ROWS // 4)
    core = me % 2
    beside = col + 1 - 2 * (col % 2)
    across = col + 2 - 4 * (col // 2)
    corner = COLS - 1 - col

    cols = pl.ds(pl.multiple_of(col * size, size), size)
    load_tok = pltpu.make_async_copy(tok_hbm.at[:, cols], tok_ref, load_sem.at[0])
    load_high = pltpu.make_async_copy(high_hbm, high_ref, load_sem.at[1])
    load_low = pltpu.make_async_copy(low_hbm, low_ref, load_sem.at[2])
    load_w = pltpu.make_async_copy(w_hbm, w_ref, load_sem.at[3])
    for load in (load_tok, load_w, load_high, load_low):
        load.start()
    barrier = pltpu.get_barrier_semaphore()
    for ahead in range(1, ROWS):
        pl.semaphore_signal(
            barrier, inc=1, device_id={"row": lax.rem(me + ahead, ROWS)}, device_id_type=MESH
        )
    for other in (beside, across, corner):
        pl.semaphore_signal(barrier, inc=1, device_id={"col": other}, device_id_type=MESH)

    lane = lax.broadcasted_iota(jnp.int32, (1, LANES), 1)
    first = lane < HALF
    cosine_lane = (lane % HALF) < QUARTER

    spot = lax.broadcasted_iota(jnp.int32, (1, size), 1)
    which = spot % HALF
    pair = (spot // HALF) * QUARTER + which % QUARTER
    partner = jnp.where(pair == 0, mid, size - pair)
    wanted = jnp.where(which < QUARTER, pair, partner)
    place = lax.broadcasted_iota(jnp.int32, (size, size), 0)
    pick = jnp.where(place == wanted, 1.0, 0.0).astype(jnp.bfloat16)
    down = lax.broadcasted_iota(jnp.int32, (size, 1), 0)
    residue = 2 * ((down % mid) // inner) + down // mid
    source = RADIX * (down % inner) + residue
    along = lax.broadcasted_iota(jnp.int32, (size, size), 1)
    order = jnp.where(along == source, 1.0, 0.0).astype(jnp.bfloat16)
    load_tok.wait()
    chosen = dot(tok_ref[...], pick).astype(jnp.bfloat16)
    ordered = dot(order, chosen)
    for tile in range(COLS):
        span = slice(tile * LANES, (tile + 1) * LANES)
        even = ordered[:mid, span]
        odd = ordered[mid:, span]
        left = jnp.where(first, even, pltpu.roll(odd, HALF, 1)).astype(jnp.bfloat16)
        right = jnp.where(first, pltpu.roll(even, HALF, 1), odd).astype(jnp.bfloat16)
        for v in range(4):
            tok_s[2 * tile, v] = left[v * inner : (v + 1) * inner]
            tok_s[2 * tile + 1, v] = right[v * inner : (v + 1) * inner]

    def token_copy(at, far, target):
        turn = at // 2
        return pltpu.make_async_remote_copy(
            src_ref=tok_s.at[at],
            dst_ref=tok_r.at[turn, :, pl.ds(pl.multiple_of(me * inner, inner), inner), :],
            send_sem=tok_send.at[at, far],
            recv_sem=tok_recv.at[turn, me],
            device_id={"row": target},
            device_id_type=MESH,
        )

    pl.semaphore_wait(barrier, ROWS - 1 + COLS - 1)

    @pl.loop(0, SLOTS)
    def _(at):
        token_copy(at, 1, row_of(at, 1 - upper)).start()
        near = row_of(at, upper)

        @pl.when(near != me)
        def _():
            token_copy(at, 0, near).start()

        @pl.when(near == me)
        def _():
            rows = pl.ds(pl.multiple_of(me * inner, inner), inner)
            for v in range(4):
                tok_r[at // 2, v, rows, :] = tok_s[at, v]

    for v in range(4):
        for start in range(0, size, LANES):
            rows = slice(start, start + LANES)
            turn_c[v, rows] = jnp.where(
                first, twist_ref[rows, 2 * v : 2 * v + 1], twist_ref[rows, 2 * v + 1 : 2 * v + 2]
            )
            turn_s[v, rows] = jnp.where(
                first,
                twist_ref[rows, RADIX + 2 * v : RADIX + 2 * v + 1],
                twist_ref[rows, RADIX + 2 * v + 1 : RADIX + 2 * v + 2],
            )

    load_high.wait()
    load_low.wait()
    load_w.wait()
    parity = lax.broadcasted_iota(jnp.int32, (EXTRA, size), 1) % 2
    swing = (1 - 2 * parity).astype(jnp.float32).astype(jnp.bfloat16)

    @pl.loop(0, groups)
    def _(g):
        side = w_ref[pl.ds(pl.multiple_of(g * size, size), size), :]
        wave = dot(high_ref[:mid], side) + dot(low_ref[:mid], side)
        sine = dot(high_ref[size : size + mid], side) + dot(low_ref[size : size + mid], side)
        last = dot(swing, side)[0:1]
        begin = pl.multiple_of(g * HALF, HALF)
        for slot in range(SLOTS):
            rows = slice(slot * QUARTER, (slot + 1) * QUARTER)
            high, low = split(wave[rows])
            fold_high[slot, pl.ds(begin, QUARTER), :] = high
            fold_low[slot, pl.ds(begin, QUARTER), :] = low
            block = -sine[rows]
            if slot == 0:
                top = lax.broadcasted_iota(jnp.int32, block.shape, 0) == 0
                block = jnp.where(top, last, block)
            high, low = split(block)
            begin_odd = pl.multiple_of(g * HALF + QUARTER, QUARTER)
            fold_high[slot, pl.ds(begin_odd, QUARTER), :] = high
            fold_low[slot, pl.ds(begin_odd, QUARTER), :] = low

    total[...] = jnp.zeros_like(total)

    def code_copy(at, quarter):
        return pltpu.make_async_remote_copy(
            src_ref=code_s.at[at // 2, quarter],
            dst_ref=gathered.at[at, col],
            send_sem=code_send.at[at // 2, quarter],
            recv_sem=code_recv.at[at],
            device_id={"row": upper * 4 + quarter},
            device_id_type=MESH,
        )

    def side_copy(at, origin, target, which):
        return pltpu.make_async_remote_copy(
            src_ref=gathered.at[at, origin],
            dst_ref=gathered.at[at, origin],
            send_sem=side_send.at[at, which],
            recv_sem=side_recv.at[at, origin],
            device_id={"col": target},
            device_id_type=MESH,
        )

    def part(turn, base):
        @pl.loop(base * 4, base * 4 + 4)
        def _(source):
            @pl.when(source != me)
            def _():
                rows = pl.ds(pl.multiple_of(source * inner, inner), inner)
                pltpu.make_async_remote_copy(
                    src_ref=tok_s.at[0],
                    dst_ref=tok_r.at[turn, :, rows, :],
                    send_sem=tok_send.at[0, 0],
                    recv_sem=tok_recv.at[turn, source],
                    device_id={"row": source},
                    device_id_type=MESH,
                ).wait_recv()

        span = pl.ds(pl.multiple_of(base * mid, mid), mid)
        terms = []
        for v in range(0, 4, 2):
            both = jnp.concatenate([tok_r[turn, v, span, :], tok_r[turn, v + 1, span, :]], axis=1)
            terms.append(dot(high_ref[:, span], both) + dot(low_ref[:, span], both))
        return terms

    def prepare(at):
        for v, term in enumerate(part(at // 2, upper)):
            found[:, 2 * v * LANES : 2 * (v + 1) * LANES] = term

    def spread(at):
        for which, target in enumerate((beside, across, corner)):
            side_copy(at, col, target, which).start()

    def produce(at):
        turn = at // 2
        for v, term in enumerate(part(turn, 1 - upper)):
            found[:, 2 * v * LANES : 2 * (v + 1) * LANES] += term

        sign = (1 - 2 * upper).astype(jnp.float32)
        lone = jnp.logical_and(lane % QUARTER == 0, at == 0)
        straight = jnp.logical_or(cosine_lane, lone)
        weights = []
        for q in range(4):
            angle = math.pi * q / 4
            weights.append(
                (
                    jnp.where(first, 1.0, sign * math.cos(angle)),
                    jnp.where(first, 0.0, sign * math.sin(angle)),
                )
            )
        tall = TALL

        def rows_of(begin):
            rows = pl.ds(begin, tall)
            lower = pl.ds(begin + size, tall)
            re, im = [], []
            for v in range(4):
                span = slice(v * LANES, (v + 1) * LANES)
                a, b = found[rows, span], found[lower, span]
                c, s = turn_c[v, rows], turn_s[v, rows]
                re.append(c * a - s * b)
                im.append(s * a + c * b)
            pr, pi = re[0] + re[2], im[0] + im[2]
            mr, mi = re[0] - re[2], im[0] - im[2]
            sr, si = re[1] + re[3], im[1] + im[3]
            dr, di = re[1] - re[3], im[1] - im[3]
            fours = [
                (pr + sr, pi + si),
                (mr - di, mi + dr),
                (pr - sr, pi - si),
                (mr + di, mi - dr),
            ]
            results = []
            for (a, b), (c, s) in zip(fours, weights):
                xr = c * a - s * b
                xi = s * a + c * b
                keep = jnp.where(straight, xr, -xi)
                move = jnp.where(lone, 0.0, jnp.where(cosine_lane, xi, xr))
                results.append(keep + pltpu.roll(move, QUARTER, 1))
            return results

        def chunk(step, peak):
            begin = pl.multiple_of(step * tall, tall)
            ones = rows_of(begin)
            twos = rows_of(pl.multiple_of(begin + mid, tall))
            for q in range(4):
                value = jnp.where(first, ones[q], twos[q]) + pltpu.roll(
                    jnp.where(first, twos[q], ones[q]), HALF, 1
                )
                packed[q, pl.ds(begin, tall), :] = value
                peak = jnp.maximum(peak, jnp.abs(value))
            return peak

        peak = jnp.zeros((tall, LANES), jnp.float32)
        peak = lax.fori_loop(0, mid // tall, chunk, peak, unroll=UNROLL)
        peak = jnp.max(peak, axis=0, keepdims=True)
        scale = jnp.broadcast_to(jnp.maximum(peak, 1e-30) * 1.0079, (EXTRA, LANES))
        scale = scale.astype(jnp.bfloat16)
        factor = CODE / scale[0:1].astype(jnp.float32)

        @pl.loop(0, 4)
        def _(q):
            block = packed[q]
            code = jnp.exp(jnp.abs(block) * factor) - 1.0
            code = jnp.where(block < 0.0, -code, code).astype(jnp.bfloat16)
            mine = upper * 4 + q == me

            @pl.when(mine)
            def _():
                gathered[at, col, :mid] = code
                gathered[at, col, mid:] = scale
                spread(at)

            @pl.when(jnp.logical_not(mine))
            def _():
                code_s[turn, q, :mid] = code
                code_s[turn, q, mid:] = scale
                code_copy(at, q).start()

    def forward(at):
        pltpu.make_async_remote_copy(
            src_ref=code_s.at[0, 0],
            dst_ref=gathered.at[at, col],
            send_sem=code_send.at[0, 0],
            recv_sem=code_recv.at[at],
            device_id={"row": row_of(at, upper)},
            device_id_type=MESH,
        ).wait_recv()
        spread(at)

    def contract(at):
        for origin in (beside, across, corner):
            side_copy(at, origin, origin, 0).wait_recv()
        tops, bottoms = [], []
        for pair_at in range(2):
            values = []
            for c in (2 * pair_at, 2 * pair_at + 1):
                factor = gathered[at, c, mid:].astype(jnp.float32)[0:1] * (scaling / CODE)
                code = gathered[at, c, :mid].astype(jnp.float32)
                value = jnp.log(1.0 + jnp.abs(code)) * factor
                values.append(jnp.where(code < 0.0, -value, value))
            tops.append(jnp.where(first, values[0], pltpu.roll(values[1], HALF, 1)))
            bottoms.append(jnp.where(first, pltpu.roll(values[0], HALF, 1), values[1]))
        for half, parts in enumerate((tops, bottoms)):
            rows = slice(half * mid, (half + 1) * mid)
            high, low = split(jnp.concatenate(parts, axis=1))
            terms = dot(high, fold_high[at]) + dot(low, fold_high[at])
            total[rows] += terms + dot(high, fold_low[at])

    def owns(at):
        return jnp.logical_and(at < SLOTS, jnp.logical_and(central, core == at % 2))

    @pl.when(owns(0))
    def _():
        prepare(0)

    @pl.loop(0, SLOTS + LATE)
    def _(step):
        @pl.when(owns(step))
        def _():
            produce(step)

        @pl.when(jnp.logical_and(step >= 1, step < SLOTS + 1))
        def _():
            @pl.when(jnp.logical_not(owns(step - 1)))
            def _():
                forward(step - 1)

        @pl.when(step >= LATE)
        def _():
            contract(step - LATE)

        @pl.when(owns(step + 1))
        def _():
            prepare(step + 1)

    out_ref[...] = total[...].astype(jnp.bfloat16)

    @pl.loop(0, SLOTS)
    def _(at):
        near = row_of(at, upper)
        token_copy(at, 1, row_of(at, 1 - upper)).wait_send()

        @pl.when(near != me)
        def _():
            token_copy(at, 0, near).wait_send()

        for which, target in enumerate((beside, across, corner)):
            side_copy(at, col, target, which).wait_send()

        @pl.when(owns(at))
        def _():
            @pl.loop(0, 4)
            def _(q):
                @pl.when(upper * 4 + q != me)
                def _():
                    code_copy(at, q).wait_send()


def kernel_body(tokens, out_weight):
    size = tokens.shape[0]
    length = size * ROWS
    scaling = 1.0 / math.sqrt(length * GROUP_DIM)
    vmem = pl.BlockSpec(memory_space=pltpu.VMEM)
    consts = [jnp.asarray(table) for table in tables(size, length)]
    bf16, f32 = jnp.bfloat16, jnp.float32
    dma = pltpu.SemaphoreType.DMA
    return pl.pallas_call(
        functools.partial(kernel, scaling),
        out_shape=jax.ShapeDtypeStruct((size, out_weight.shape[1]), bf16),
        in_specs=[pl.BlockSpec(memory_space=pl.ANY)] * 4 + [vmem],
        out_specs=vmem,
        scratch_shapes=[
            pltpu.VMEM((size, size), bf16),
            pltpu.VMEM(out_weight.shape, bf16),
            pltpu.VMEM((2 * size, size), bf16),
            pltpu.VMEM((2 * size, size), bf16),
            pltpu.VMEM((SLOTS, 4, size // RADIX, LANES), bf16),
            pltpu.VMEM((4, 4, size, LANES), bf16),
            pltpu.VMEM((4, size, LANES), f32),
            pltpu.VMEM((4, size, LANES), f32),
            pltpu.VMEM((2 * size, 4 * LANES), f32),
            pltpu.VMEM((4, size // 2, LANES), f32),
            pltpu.VMEM((4, 4, size // 2 + EXTRA, LANES), bf16),
            pltpu.VMEM((SLOTS, COLS, size // 2 + EXTRA, LANES), bf16),
            pltpu.VMEM((SLOTS, COLS * HALF, out_weight.shape[1]), bf16),
            pltpu.VMEM((SLOTS, COLS * HALF, out_weight.shape[1]), bf16),
            pltpu.VMEM((size, out_weight.shape[1]), f32),
            dma((4,)),
            dma((SLOTS, 2)),
            dma((4, ROWS)),
            dma((4, 4)),
            dma((SLOTS,)),
            dma((SLOTS, 3)),
            dma((SLOTS, COLS)),
        ],
        compiler_params=pltpu.CompilerParams(
            collective_id=0, has_side_effects=True, vmem_limit_bytes=60 * 1024 * 1024
        ),
    )(tokens, out_weight, *consts)


def body(tokens, out_weight):
    size = tokens.shape[0]
    fits = (
        lax.axis_size("row") == ROWS
        and lax.axis_size("col") == COLS
        and size == GROUP_DIM
        and tokens.shape[1] == COLS * GROUP_DIM
        and out_weight.shape[1] == GROUP_DIM
    )
    if fits:
        return kernel_body(tokens, out_weight)
    return general_body(tokens, out_weight)


def solution(mesh):
    placed = (P("row", None), P(None, "col"))
    return jax.shard_map(
        body, mesh=mesh, in_specs=placed, out_specs=P("row", "col"), check_vma=False
    )
```

```python
import math

import functools

import jax
import jax.numpy as jnp
import numpy as np
from jax import lax
from jax.experimental import pallas as pl
from jax.experimental.pallas import tpu as pltpu
from jax.sharding import PartitionSpec as P

GROUPS = 4
GROUP_DIM = 512


def angles(product, period):
    return (product % period).astype(jnp.float32) * (2.0 * math.pi / period)


def plain_dot(matrix, values):
    return jnp.dot(
        matrix, values, precision=lax.Precision.HIGHEST, preferred_element_type=jnp.float32
    )


def whole_transform(whole_rows, row_count, seg_rows, length):
    few_chans = whole_rows.shape[2]
    lattice = jnp.arange(row_count, dtype=jnp.int32)
    phases = angles(lattice[:, None] * lattice[None, :], row_count)
    cosine_table = jnp.cos(phases)
    sine_table = jnp.sin(phases)
    real_in = whole_rows[0].reshape(row_count, seg_rows * few_chans)
    imag_in = whole_rows[1].reshape(row_count, seg_rows * few_chans)
    first_re = (plain_dot(cosine_table, real_in) + plain_dot(sine_table, imag_in)).reshape(
        row_count, seg_rows, few_chans
    )
    first_im = (plain_dot(cosine_table, imag_in) - plain_dot(sine_table, real_in)).reshape(
        row_count, seg_rows, few_chans
    )
    inner = jnp.arange(seg_rows, dtype=jnp.int32)
    twist = angles(lattice[:, None] * inner[None, :], length)[:, :, None]
    twist_cos = jnp.cos(twist)
    twist_sin = jnp.sin(twist)
    turned_re = twist_cos * first_re + twist_sin * first_im
    turned_im = twist_cos * first_im - twist_sin * first_re
    folded_re = jnp.transpose(turned_re, (1, 0, 2)).reshape(seg_rows, row_count * few_chans)
    folded_im = jnp.transpose(turned_im, (1, 0, 2)).reshape(seg_rows, row_count * few_chans)
    seg_phases = angles(inner[:, None] * inner[None, :], seg_rows)
    real_part = plain_dot(jnp.cos(seg_phases), folded_re) + plain_dot(
        jnp.sin(seg_phases), folded_im
    )
    return real_part.reshape(length, few_chans)


def general_body(tokens, out_weight):
    seg_rows = tokens.shape[0]
    col_width = out_weight.shape[1]
    row_count = lax.axis_size("row")
    length = seg_rows * row_count
    scaling = 1.0 / math.sqrt(length * GROUP_DIM)
    weight_wide = out_weight.astype(jnp.float32)
    lattice = jnp.arange(GROUP_DIM, dtype=jnp.int32)
    phases = angles(lattice[:, None] * lattice[None, :], GROUP_DIM)
    cosine_table = jnp.cos(phases) * scaling
    sine_table = jnp.sin(phases) * scaling
    folded_rows = []
    for group in range(GROUPS):
        group_rows = weight_wide[group * GROUP_DIM : (group + 1) * GROUP_DIM]
        folded_rows.append(
            jnp.concatenate(
                [plain_dot(cosine_table, group_rows), -plain_dot(sine_table, group_rows)], axis=1
            )
        )
    folded_map = jnp.concatenate(folded_rows, axis=0)
    spectrum = plain_dot(tokens.astype(jnp.float32), folded_map)
    stacked = jnp.stack([spectrum[:, :col_width], spectrum[:, col_width:]])
    whole_rows = lax.all_to_all(stacked, "row", split_axis=2, concat_axis=1, tiled=True)
    ordered = whole_transform(whole_rows, row_count, seg_rows, length)
    spectral = lax.all_to_all(
        ordered.astype(jnp.bfloat16), "row", split_axis=0, concat_axis=1, tiled=True
    )
    return spectral

RADIX = 8
HALF = 64
QUARTER = 32
LANES = 128
EXTRA = 16
ROWS = 8
COLS = 4
SLOTS = 8
CODE = 84.0
LATE = 5
LATER = 3
INNER = 6
OUTER = 6
TALL = 32
UNROLL = 4
MESH = pl.DeviceIdType.MESH


def split_table(values):
    big = values.astype(jnp.bfloat16)
    return big, (values - big.astype(np.float64)).astype(jnp.bfloat16)


def tables(size, length):
    index = np.arange(size)
    phase = 2.0 * np.pi * ((index[:, None] * index[None, :]) % size) / size
    high, low = split_table(np.concatenate([np.cos(phase), np.sin(phase)], axis=0))
    turn = 2.0 * np.pi * (index[:, None] * np.arange(RADIX)[None, :]) / length
    twist = np.zeros((size, LANES), np.float32)
    twist[:, :RADIX] = np.cos(turn)
    twist[:, RADIX : 2 * RADIX] = np.sin(turn)
    return high, low, twist


def dot(a, b):
    return jnp.dot(a, b, preferred_element_type=jnp.float32)


def split(values):
    high = values.astype(jnp.bfloat16)
    return high, (values - high.astype(jnp.float32)).astype(jnp.bfloat16)


def row_of(slot, upper):
    return ROWS // 4 + upper * (ROWS // 4) + slot % 2


def kernel(
    scaling,
    tok_hbm,
    w_hbm,
    high_hbm,
    low_hbm,
    twist_hbm,
    out_ref,
    tok_ref,
    w_ref,
    high_ref,
    low_ref,
    twist_ref,
    tok_s,
    tok_r,
    turn_c,
    turn_s,
    found,
    packed,
    code_s,
    gathered,
    fold_high,
    fold_low,
    total,
    load_sem,
    tok_send,
    tok_recv,
    code_send,
    code_recv,
    side_send,
    side_recv,
):
    me = lax.axis_index("row")
    col = lax.axis_index("col")
    size = tok_ref.shape[0]
    inner = size // RADIX
    mid = size // 2
    groups = COLS
    upper = me // (ROWS // 2)
    central = jnp.logical_and(me >= ROWS // 4, me < 3 * ROWS // 4)
    core = me % 2
    beside = col + 1 - 2 * (col % 2)
    across = col + 2 - 4 * (col // 2)
    corner = COLS - 1 - col

    cols = pl.ds(pl.multiple_of(col * size, size), size)
    load_tok = pltpu.make_async_copy(tok_hbm.at[:, cols], tok_ref, load_sem.at[0])
    load_high = pltpu.make_async_copy(high_hbm, high_ref, load_sem.at[1])
    load_low = pltpu.make_async_copy(low_hbm, low_ref, load_sem.at[2])
    load_w = pltpu.make_async_copy(w_hbm, w_ref, load_sem.at[3])
    load_twist = pltpu.make_async_copy(twist_hbm, twist_ref, load_sem.at[4])
    load_tok.start()
    barrier = pltpu.get_barrier_semaphore()
    for ahead in range(1, ROWS):
        pl.semaphore_signal(
            barrier, inc=1, device_id={"row": lax.rem(me + ahead, ROWS)}, device_id_type=MESH
        )
    for other in (beside, across, corner):
        pl.semaphore_signal(barrier, inc=1, device_id={"col": other}, device_id_type=MESH)

    for load in (load_twist, load_high, load_low, load_w):
        load.start()

    lane = lax.broadcasted_iota(jnp.int32, (1, LANES), 1)
    first = lane < HALF
    cosine_lane = (lane % HALF) < QUARTER

    spot = lax.broadcasted_iota(jnp.int32, (1, size), 1)
    which = spot % HALF
    pair = (spot // HALF) * QUARTER + which % QUARTER
    partner = jnp.where(pair == 0, mid, size - pair)
    wanted = jnp.where(which < QUARTER, pair, partner)
    place = lax.broadcasted_iota(jnp.int32, (size, size), 0)
    pick = jnp.where(place == wanted, 1.0, 0.0).astype(jnp.bfloat16)
    down = lax.broadcasted_iota(jnp.int32, (size, 1), 0)
    residue = 2 * ((down % mid) // inner) + down // mid
    source = RADIX * (down % inner) + residue
    along = lax.broadcasted_iota(jnp.int32, (size, size), 1)
    order = jnp.where(along == source, 1.0, 0.0).astype(jnp.bfloat16)
    def token_copy(at, far, target):
        turn = at // 2
        return pltpu.make_async_remote_copy(
            src_ref=tok_s.at[at],
            dst_ref=tok_r.at[turn, :, pl.ds(pl.multiple_of(me * inner, inner), inner), :],
            send_sem=tok_send.at[at, far],
            recv_sem=tok_recv.at[turn, me],
            device_id={"row": target},
            device_id_type=MESH,
        )

    load_tok.wait()
    for tile in range(COLS):
        span = slice(tile * LANES, (tile + 1) * LANES)
        chosen = dot(tok_ref[...], pick[:, span]).astype(jnp.bfloat16)
        ordered = dot(order, chosen)
        even = ordered[:mid]
        odd = ordered[mid:]
        left = jnp.where(first, even, pltpu.roll(odd, HALF, 1)).astype(jnp.bfloat16)
        right = jnp.where(first, pltpu.roll(even, HALF, 1), odd).astype(jnp.bfloat16)
        for v in range(4):
            tok_s[2 * tile, v] = left[v * inner : (v + 1) * inner]
            tok_s[2 * tile + 1, v] = right[v * inner : (v + 1) * inner]
        if tile == 0:
            pl.semaphore_wait(barrier, ROWS - 1 + COLS - 1)

        @pl.loop(2 * tile, 2 * tile + 2)
        def _(at):
            near = row_of(at, upper)

            @pl.when(near != me)
            def _():
                token_copy(at, 0, near).start()

            token_copy(at, 1, row_of(at, 1 - upper)).start()

            @pl.when(near == me)
            def _():
                rows = pl.ds(pl.multiple_of(me * inner, inner), inner)
                for v in range(4):
                    tok_r[at // 2, v, rows, :] = tok_s[at, v]

    load_twist.wait()
    for v in range(4):
        for start in range(0, size, LANES):
            rows = slice(start, start + LANES)
            turn_c[v, rows] = jnp.where(
                first, twist_ref[rows, 2 * v : 2 * v + 1], twist_ref[rows, 2 * v + 1 : 2 * v + 2]
            )
            turn_s[v, rows] = jnp.where(
                first,
                twist_ref[rows, RADIX + 2 * v : RADIX + 2 * v + 1],
                twist_ref[rows, RADIX + 2 * v + 1 : RADIX + 2 * v + 2],
            )

    parity = lax.broadcasted_iota(jnp.int32, (EXTRA, size), 1) % 2
    swing = (1 - 2 * parity).astype(jnp.float32).astype(jnp.bfloat16)

    def fold(g):
        side = w_ref[pl.ds(pl.multiple_of(g * size, size), size), :]
        wave = dot(high_ref[:mid], side) + dot(low_ref[:mid], side)
        sine = dot(high_ref[size : size + mid], side) + dot(low_ref[size : size + mid], side)
        last = dot(swing, side)[0:1]
        begin = pl.multiple_of(g * HALF, HALF)
        for slot in range(SLOTS):
            rows = slice(slot * QUARTER, (slot + 1) * QUARTER)
            high, low = split(wave[rows])
            fold_high[slot, pl.ds(begin, QUARTER), :] = high
            fold_low[slot, pl.ds(begin, QUARTER), :] = low
            block = -sine[rows]
            if slot == 0:
                top = lax.broadcasted_iota(jnp.int32, block.shape, 0) == 0
                block = jnp.where(top, last, block)
            high, low = split(block)
            begin_odd = pl.multiple_of(g * HALF + QUARTER, QUARTER)
            fold_high[slot, pl.ds(begin_odd, QUARTER), :] = high
            fold_low[slot, pl.ds(begin_odd, QUARTER), :] = low

    total[...] = jnp.zeros_like(total)

    def code_copy(at, quarter):
        return pltpu.make_async_remote_copy(
            src_ref=code_s.at[at // 2, quarter],
            dst_ref=gathered.at[at, col],
            send_sem=code_send.at[at // 2, quarter],
            recv_sem=code_recv.at[at],
            device_id={"row": upper * 4 + quarter},
            device_id_type=MESH,
        )

    def side_copy(at, origin, target, which):
        return pltpu.make_async_remote_copy(
            src_ref=gathered.at[at, origin],
            dst_ref=gathered.at[at, origin],
            send_sem=side_send.at[at, which],
            recv_sem=side_recv.at[at, origin],
            device_id={"col": target},
            device_id_type=MESH,
        )

    def part(turn, base):
        @pl.loop(base * 4, base * 4 + 4)
        def _(source):
            @pl.when(source != me)
            def _():
                rows = pl.ds(pl.multiple_of(source * inner, inner), inner)
                pltpu.make_async_remote_copy(
                    src_ref=tok_s.at[0],
                    dst_ref=tok_r.at[turn, :, rows, :],
                    send_sem=tok_send.at[0, 0],
                    recv_sem=tok_recv.at[turn, source],
                    device_id={"row": source},
                    device_id_type=MESH,
                ).wait_recv()

        span = pl.ds(pl.multiple_of(base * mid, mid), mid)
        terms = []
        for v in range(0, 4, 2):
            both = jnp.concatenate([tok_r[turn, v, span, :], tok_r[turn, v + 1, span, :]], axis=1)
            terms.append(dot(high_ref[:, span], both) + dot(low_ref[:, span], both))
        return terms

    def prepare(at):
        for v, term in enumerate(part(at // 2, upper)):
            found[:, 2 * v * LANES : 2 * (v + 1) * LANES] = term

    relayed = jnp.where(central, INNER, OUTER)

    def spread(at):
        side_copy(at, col, beside, 0).start()
        side_copy(at, col, across, 1).start()

        @pl.when(at >= relayed)
        def _():
            side_copy(at, col, corner, 2).start()

    via = beside + core * (across - beside)
    onward = across + core * (beside - across)

    def relay(at):
        side_copy(at, via, via, 2).wait_recv()
        side_copy(at, via, onward, 2).start()

    def finish(at):
        for v, term in enumerate(part(at // 2, 1 - upper)):
            found[:, 2 * v * LANES : 2 * (v + 1) * LANES] += term

    def produce(at):
        turn = at // 2
        sign = (1 - 2 * upper).astype(jnp.float32)
        lone = jnp.logical_and(lane % QUARTER == 0, at == 0)
        straight = jnp.logical_or(cosine_lane, lone)
        weights = []
        for q in range(4):
            angle = math.pi * q / 4
            weights.append(
                (
                    jnp.where(first, 1.0, sign * math.cos(angle)),
                    jnp.where(first, 0.0, sign * math.sin(angle)),
                )
            )
        tall = TALL

        def rows_of(begin):
            rows = pl.ds(begin, tall)
            lower = pl.ds(begin + size, tall)
            re, im = [], []
            for v in range(4):
                span = slice(v * LANES, (v + 1) * LANES)
                a, b = found[rows, span], found[lower, span]
                c, s = turn_c[v, rows], turn_s[v, rows]
                re.append(c * a - s * b)
                im.append(s * a + c * b)
            pr, pi = re[0] + re[2], im[0] + im[2]
            mr, mi = re[0] - re[2], im[0] - im[2]
            sr, si = re[1] + re[3], im[1] + im[3]
            dr, di = re[1] - re[3], im[1] - im[3]
            fours = [
                (pr + sr, pi + si),
                (mr - di, mi + dr),
                (pr - sr, pi - si),
                (mr + di, mi - dr),
            ]
            results = []
            for (a, b), (c, s) in zip(fours, weights):
                xr = c * a - s * b
                xi = s * a + c * b
                keep = jnp.where(straight, xr, -xi)
                move = jnp.where(lone, 0.0, jnp.where(cosine_lane, xi, xr))
                results.append(keep + pltpu.roll(move, QUARTER, 1))
            return results

        def chunk(step, peak):
            begin = pl.multiple_of(step * tall, tall)
            ones = rows_of(begin)
            twos = rows_of(pl.multiple_of(begin + mid, tall))
            for q in range(4):
                value = jnp.where(first, ones[q], twos[q]) + pltpu.roll(
                    jnp.where(first, twos[q], ones[q]), HALF, 1
                )
                packed[q, pl.ds(begin, tall), :] = value
                peak = jnp.maximum(peak, jnp.abs(value))
            return peak

        peak = jnp.zeros((tall, LANES), jnp.float32)
        peak = lax.fori_loop(0, mid // tall, chunk, peak, unroll=UNROLL)
        peak = jnp.max(peak, axis=0, keepdims=True)
        scale = jnp.broadcast_to(jnp.maximum(peak, 1e-30) * 1.0079, (EXTRA, LANES))
        scale = scale.astype(jnp.bfloat16)
        factor = CODE / scale[0:1].astype(jnp.float32)

        @pl.loop(0, 4)
        def _(turn_at):
            q = lax.rem(turn_at + 2 * upper, 4)
            block = packed[q]
            code = jnp.exp(jnp.abs(block) * factor) - 1.0
            code = jnp.where(block < 0.0, -code, code).astype(jnp.bfloat16)
            mine = upper * 4 + q == me

            @pl.when(mine)
            def _():
                gathered[at, col, :mid] = code
                gathered[at, col, mid:] = scale
                spread(at)

            @pl.when(jnp.logical_not(mine))
            def _():
                code_s[turn, q, :mid] = code
                code_s[turn, q, mid:] = scale
                code_copy(at, q).start()

    def forward(at):
        pltpu.make_async_remote_copy(
            src_ref=code_s.at[0, 0],
            dst_ref=gathered.at[at, col],
            send_sem=code_send.at[0, 0],
            recv_sem=code_recv.at[at],
            device_id={"row": row_of(at, upper)},
            device_id_type=MESH,
        ).wait_recv()
        spread(at)

    def contract(at):
        for origin in (onward, corner):
            side_copy(at, origin, origin, 0).wait_recv()

        @pl.when(at >= relayed)
        def _():
            side_copy(at, via, via, 0).wait_recv()

        tops, bottoms = [], []
        for pair_at in range(2):
            values = []
            for c in (2 * pair_at, 2 * pair_at + 1):
                factor = gathered[at, c, mid:].astype(jnp.float32)[0:1] * (scaling / CODE)
                code = gathered[at, c, :mid].astype(jnp.float32)
                value = jnp.log(1.0 + jnp.abs(code)) * factor
                values.append(jnp.where(code < 0.0, -value, value))
            tops.append(jnp.where(first, values[0], pltpu.roll(values[1], HALF, 1)))
            bottoms.append(jnp.where(first, pltpu.roll(values[0], HALF, 1), values[1]))
        for half, parts in enumerate((tops, bottoms)):
            rows = slice(half * mid, (half + 1) * mid)
            high, low = split(jnp.concatenate(parts, axis=1))
            terms = dot(high, fold_high[at]) + dot(low, fold_high[at])
            total[rows] += terms + dot(high, fold_low[at])

    def owns(at):
        return jnp.logical_and(at < SLOTS, jnp.logical_and(central, core == at % 2))

    load_high.wait()
    load_low.wait()
    load_w.wait()

    @pl.when(owns(0))
    def _():
        prepare(0)

    @pl.loop(0, SLOTS + LATE)
    def _(step):
        @pl.when(owns(step))
        def _():
            finish(step)

        @pl.when(jnp.logical_and(step >= LATER, step < relayed + LATER))
        def _():
            relay(step - LATER)

        @pl.when(jnp.logical_and(step >= 1, step < SLOTS + 1))
        def _():
            @pl.when(jnp.logical_not(owns(step - 1)))
            def _():
                forward(step - 1)

        @pl.when(owns(step))
        def _():
            produce(step)

        @pl.when(step >= LATE)
        def _():
            contract(step - LATE)

        @pl.when(step < groups)
        def _():
            fold(step)

        @pl.when(owns(step + 1))
        def _():
            prepare(step + 1)

    out_ref[...] = total[...].astype(jnp.bfloat16)

    @pl.loop(0, SLOTS)
    def _(at):
        near = row_of(at, upper)
        token_copy(at, 1, row_of(at, 1 - upper)).wait_send()

        @pl.when(near != me)
        def _():
            token_copy(at, 0, near).wait_send()

        for which, target in enumerate((beside, across, corner)):
            side_copy(at, col, target, which).wait_send()

        @pl.when(owns(at))
        def _():
            @pl.loop(0, 4)
            def _(q):
                @pl.when(upper * 4 + q != me)
                def _():
                    code_copy(at, q).wait_send()


def kernel_body(tokens, out_weight):
    size = tokens.shape[0]
    length = size * ROWS
    scaling = 1.0 / math.sqrt(length * GROUP_DIM)
    vmem = pl.BlockSpec(memory_space=pltpu.VMEM)
    consts = [jnp.asarray(table) for table in tables(size, length)]
    bf16, f32 = jnp.bfloat16, jnp.float32
    dma = pltpu.SemaphoreType.DMA
    return pl.pallas_call(
        functools.partial(kernel, scaling),
        out_shape=jax.ShapeDtypeStruct((size, out_weight.shape[1]), bf16),
        in_specs=[pl.BlockSpec(memory_space=pl.ANY)] * 5,
        out_specs=vmem,
        scratch_shapes=[
            pltpu.VMEM((size, size), bf16),
            pltpu.VMEM(out_weight.shape, bf16),
            pltpu.VMEM((2 * size, size), bf16),
            pltpu.VMEM((2 * size, size), bf16),
            pltpu.VMEM((size, LANES), f32),
            pltpu.VMEM((SLOTS, 4, size // RADIX, LANES), bf16),
            pltpu.VMEM((4, 4, size, LANES), bf16),
            pltpu.VMEM((4, size, LANES), f32),
            pltpu.VMEM((4, size, LANES), f32),
            pltpu.VMEM((2 * size, 4 * LANES), f32),
            pltpu.VMEM((4, size // 2, LANES), f32),
            pltpu.VMEM((4, 4, size // 2 + EXTRA, LANES), bf16),
            pltpu.VMEM((SLOTS, COLS, size // 2 + EXTRA, LANES), bf16),
            pltpu.VMEM((SLOTS, COLS * HALF, out_weight.shape[1]), bf16),
            pltpu.VMEM((SLOTS, COLS * HALF, out_weight.shape[1]), bf16),
            pltpu.VMEM((size, out_weight.shape[1]), f32),
            dma((5,)),
            dma((SLOTS, 2)),
            dma((4, ROWS)),
            dma((4, 4)),
            dma((SLOTS,)),
            dma((SLOTS, 3)),
            dma((SLOTS, COLS)),
        ],
        compiler_params=pltpu.CompilerParams(
            collective_id=0, has_side_effects=True, vmem_limit_bytes=60 * 1024 * 1024
        ),
    )(tokens, out_weight, *consts)


def body(tokens, out_weight):
    size = tokens.shape[0]
    fits = (
        lax.axis_size("row") == ROWS
        and lax.axis_size("col") == COLS
        and size == GROUP_DIM
        and tokens.shape[1] == COLS * GROUP_DIM
        and out_weight.shape[1] == GROUP_DIM
    )
    if fits:
        return kernel_body(tokens, out_weight)
    return general_body(tokens, out_weight)


def solution(mesh):
    placed = (P("row", None), P(None, "col"))
    return jax.shard_map(
        body, mesh=mesh, in_specs=placed, out_specs=P("row", "col"), check_vma=False
    )
```

```python
import math

import functools

import jax
import jax.numpy as jnp
import numpy as np
from jax import lax
from jax.experimental import pallas as pl
from jax.experimental.pallas import tpu as pltpu
from jax.sharding import PartitionSpec as P

GROUPS = 4
GROUP_DIM = 512


def angles(product, period):
    return (product % period).astype(jnp.float32) * (2.0 * math.pi / period)


def plain_dot(matrix, values):
    return jnp.dot(
        matrix, values, precision=lax.Precision.HIGHEST, preferred_element_type=jnp.float32
    )


def whole_transform(whole_rows, row_count, seg_rows, length):
    few_chans = whole_rows.shape[2]
    lattice = jnp.arange(row_count, dtype=jnp.int32)
    phases = angles(lattice[:, None] * lattice[None, :], row_count)
    cosine_table = jnp.cos(phases)
    sine_table = jnp.sin(phases)
    real_in = whole_rows[0].reshape(row_count, seg_rows * few_chans)
    imag_in = whole_rows[1].reshape(row_count, seg_rows * few_chans)
    first_re = (plain_dot(cosine_table, real_in) + plain_dot(sine_table, imag_in)).reshape(
        row_count, seg_rows, few_chans
    )
    first_im = (plain_dot(cosine_table, imag_in) - plain_dot(sine_table, real_in)).reshape(
        row_count, seg_rows, few_chans
    )
    inner = jnp.arange(seg_rows, dtype=jnp.int32)
    twist = angles(lattice[:, None] * inner[None, :], length)[:, :, None]
    twist_cos = jnp.cos(twist)
    twist_sin = jnp.sin(twist)
    turned_re = twist_cos * first_re + twist_sin * first_im
    turned_im = twist_cos * first_im - twist_sin * first_re
    folded_re = jnp.transpose(turned_re, (1, 0, 2)).reshape(seg_rows, row_count * few_chans)
    folded_im = jnp.transpose(turned_im, (1, 0, 2)).reshape(seg_rows, row_count * few_chans)
    seg_phases = angles(inner[:, None] * inner[None, :], seg_rows)
    real_part = plain_dot(jnp.cos(seg_phases), folded_re) + plain_dot(
        jnp.sin(seg_phases), folded_im
    )
    return real_part.reshape(length, few_chans)


def general_body(tokens, out_weight):
    seg_rows = tokens.shape[0]
    col_width = out_weight.shape[1]
    row_count = lax.axis_size("row")
    length = seg_rows * row_count
    scaling = 1.0 / math.sqrt(length * GROUP_DIM)
    weight_wide = out_weight.astype(jnp.float32)
    lattice = jnp.arange(GROUP_DIM, dtype=jnp.int32)
    phases = angles(lattice[:, None] * lattice[None, :], GROUP_DIM)
    cosine_table = jnp.cos(phases) * scaling
    sine_table = jnp.sin(phases) * scaling
    folded_rows = []
    for group in range(GROUPS):
        group_rows = weight_wide[group * GROUP_DIM : (group + 1) * GROUP_DIM]
        folded_rows.append(
            jnp.concatenate(
                [plain_dot(cosine_table, group_rows), -plain_dot(sine_table, group_rows)], axis=1
            )
        )
    folded_map = jnp.concatenate(folded_rows, axis=0)
    spectrum = plain_dot(tokens.astype(jnp.float32), folded_map)
    stacked = jnp.stack([spectrum[:, :col_width], spectrum[:, col_width:]])
    whole_rows = lax.all_to_all(stacked, "row", split_axis=2, concat_axis=1, tiled=True)
    ordered = whole_transform(whole_rows, row_count, seg_rows, length)
    spectral = lax.all_to_all(
        ordered.astype(jnp.bfloat16), "row", split_axis=0, concat_axis=1, tiled=True
    )
    return spectral

RADIX = 8
HALF = 64
QUARTER = 32
LANES = 128
EXTRA = 16
ROWS = 8
COLS = 4
SLOTS = 8
CODE = 84.0
LATE = 5
LATER = 3
INNER = 7
OUTER = 6
TALL = 32
UNROLL = 4
MESH = pl.DeviceIdType.MESH


def split_table(values):
    big = values.astype(jnp.bfloat16)
    return big, (values - big.astype(np.float64)).astype(jnp.bfloat16)


def tables(size, length):
    index = np.arange(size)
    phase = 2.0 * np.pi * ((index[:, None] * index[None, :]) % size) / size
    high, low = split_table(np.concatenate([np.cos(phase), np.sin(phase)], axis=0))
    turn = 2.0 * np.pi * (index[:, None] * np.arange(RADIX)[None, :]) / length
    twist = np.zeros((size, LANES), np.float32)
    twist[:, :RADIX] = np.cos(turn)
    twist[:, RADIX : 2 * RADIX] = np.sin(turn)
    return high, low, twist


def dot(a, b):
    return jnp.dot(a, b, preferred_element_type=jnp.float32)


def split(values):
    high = values.astype(jnp.bfloat16)
    return high, (values - high.astype(jnp.float32)).astype(jnp.bfloat16)


def row_of(slot, upper):
    return ROWS // 4 + upper * (ROWS // 4) + slot % 2


def kernel(
    scaling,
    tok_hbm,
    w_hbm,
    high_hbm,
    low_hbm,
    twist_hbm,
    out_ref,
    tok_ref,
    w_ref,
    high_ref,
    low_ref,
    twist_ref,
    tok_s,
    tok_r,
    turn_c,
    turn_s,
    found,
    packed,
    code_s,
    gathered,
    fold_high,
    fold_low,
    total,
    load_sem,
    tok_send,
    tok_recv,
    code_send,
    code_recv,
    side_send,
    side_recv,
):
    me = lax.axis_index("row")
    col = lax.axis_index("col")
    size = tok_ref.shape[0]
    inner = size // RADIX
    mid = size // 2
    groups = COLS
    upper = me // (ROWS // 2)
    central = jnp.logical_and(me >= ROWS // 4, me < 3 * ROWS // 4)
    core = me % 2
    beside = col + 1 - 2 * (col % 2)
    across = col + 2 - 4 * (col // 2)
    corner = COLS - 1 - col

    cols = pl.ds(pl.multiple_of(col * size, size), size)
    load_tok = pltpu.make_async_copy(tok_hbm.at[:, cols], tok_ref, load_sem.at[0])
    load_high = pltpu.make_async_copy(high_hbm, high_ref, load_sem.at[1])
    load_low = pltpu.make_async_copy(low_hbm, low_ref, load_sem.at[2])
    load_w = pltpu.make_async_copy(w_hbm, w_ref, load_sem.at[3])
    load_twist = pltpu.make_async_copy(twist_hbm, twist_ref, load_sem.at[4])
    load_tok.start()
    barrier = pltpu.get_barrier_semaphore()
    for ahead in range(1, ROWS):
        pl.semaphore_signal(
            barrier, inc=1, device_id={"row": lax.rem(me + ahead, ROWS)}, device_id_type=MESH
        )
    for other in (beside, across, corner):
        pl.semaphore_signal(barrier, inc=1, device_id={"col": other}, device_id_type=MESH)

    for load in (load_twist, load_high, load_low, load_w):
        load.start()

    lane = lax.broadcasted_iota(jnp.int32, (1, LANES), 1)
    first = lane < HALF
    cosine_lane = (lane % HALF) < QUARTER

    spot = lax.broadcasted_iota(jnp.int32, (1, size), 1)
    which = spot % HALF
    pair = (spot // HALF) * QUARTER + which % QUARTER
    partner = jnp.where(pair == 0, mid, size - pair)
    wanted = jnp.where(which < QUARTER, pair, partner)
    place = lax.broadcasted_iota(jnp.int32, (size, size), 0)
    pick = jnp.where(place == wanted, 1.0, 0.0).astype(jnp.bfloat16)
    down = lax.broadcasted_iota(jnp.int32, (size, 1), 0)
    residue = 2 * ((down % mid) // inner) + down // mid
    source = RADIX * (down % inner) + residue
    along = lax.broadcasted_iota(jnp.int32, (size, size), 1)
    order = jnp.where(along == source, 1.0, 0.0).astype(jnp.bfloat16)
    def token_copy(at, far, target):
        turn = at // 2
        return pltpu.make_async_remote_copy(
            src_ref=tok_s.at[at],
            dst_ref=tok_r.at[turn, :, pl.ds(pl.multiple_of(me * inner, inner), inner), :],
            send_sem=tok_send.at[at, far],
            recv_sem=tok_recv.at[turn, me],
            device_id={"row": target},
            device_id_type=MESH,
        )

    load_tok.wait()
    for tile in range(COLS):
        span = slice(tile * LANES, (tile + 1) * LANES)
        chosen = dot(tok_ref[...], pick[:, span]).astype(jnp.bfloat16)
        ordered = dot(order, chosen)
        even = ordered[:mid]
        odd = ordered[mid:]
        left = jnp.where(first, even, pltpu.roll(odd, HALF, 1)).astype(jnp.bfloat16)
        right = jnp.where(first, pltpu.roll(even, HALF, 1), odd).astype(jnp.bfloat16)
        for v in range(4):
            tok_s[2 * tile, v] = left[v * inner : (v + 1) * inner]
            tok_s[2 * tile + 1, v] = right[v * inner : (v + 1) * inner]
        if tile == 0:
            pl.semaphore_wait(barrier, ROWS - 1 + COLS - 1)

        @pl.loop(2 * tile, 2 * tile + 2)
        def _(at):
            near = row_of(at, upper)

            @pl.when(near != me)
            def _():
                token_copy(at, 0, near).start()

            token_copy(at, 1, row_of(at, 1 - upper)).start()

            @pl.when(near == me)
            def _():
                rows = pl.ds(pl.multiple_of(me * inner, inner), inner)
                for v in range(4):
                    tok_r[at // 2, v, rows, :] = tok_s[at, v]

    load_twist.wait()
    for v in range(4):
        for start in range(0, size, LANES):
            rows = slice(start, start + LANES)
            turn_c[v, rows] = jnp.where(
                first, twist_ref[rows, 2 * v : 2 * v + 1], twist_ref[rows, 2 * v + 1 : 2 * v + 2]
            )
            turn_s[v, rows] = jnp.where(
                first,
                twist_ref[rows, RADIX + 2 * v : RADIX + 2 * v + 1],
                twist_ref[rows, RADIX + 2 * v + 1 : RADIX + 2 * v + 2],
            )

    parity = lax.broadcasted_iota(jnp.int32, (EXTRA, size), 1) % 2
    swing = (1 - 2 * parity).astype(jnp.float32).astype(jnp.bfloat16)

    def fold(g):
        side = w_ref[pl.ds(pl.multiple_of(g * size, size), size), :]
        wave = dot(high_ref[:mid], side) + dot(low_ref[:mid], side)
        sine = dot(high_ref[size : size + mid], side) + dot(low_ref[size : size + mid], side)
        last = dot(swing, side)[0:1]
        begin = pl.multiple_of(g * HALF, HALF)
        for slot in range(SLOTS):
            rows = slice(slot * QUARTER, (slot + 1) * QUARTER)
            high, low = split(wave[rows])
            fold_high[slot, pl.ds(begin, QUARTER), :] = high
            fold_low[slot, pl.ds(begin, QUARTER), :] = low
            block = -sine[rows]
            if slot == 0:
                top = lax.broadcasted_iota(jnp.int32, block.shape, 0) == 0
                block = jnp.where(top, last, block)
            high, low = split(block)
            begin_odd = pl.multiple_of(g * HALF + QUARTER, QUARTER)
            fold_high[slot, pl.ds(begin_odd, QUARTER), :] = high
            fold_low[slot, pl.ds(begin_odd, QUARTER), :] = low

    total[...] = jnp.zeros_like(total)

    def code_copy(at, quarter):
        return pltpu.make_async_remote_copy(
            src_ref=code_s.at[at // 2, quarter],
            dst_ref=gathered.at[at, col],
            send_sem=code_send.at[at // 2, quarter],
            recv_sem=code_recv.at[at],
            device_id={"row": upper * 4 + quarter},
            device_id_type=MESH,
        )

    def side_copy(at, origin, target, which):
        return pltpu.make_async_remote_copy(
            src_ref=gathered.at[at, origin],
            dst_ref=gathered.at[at, origin],
            send_sem=side_send.at[at, which],
            recv_sem=side_recv.at[at, origin],
            device_id={"col": target},
            device_id_type=MESH,
        )

    def part(turn, base):
        @pl.loop(base * 4, base * 4 + 4)
        def _(source):
            @pl.when(source != me)
            def _():
                rows = pl.ds(pl.multiple_of(source * inner, inner), inner)
                pltpu.make_async_remote_copy(
                    src_ref=tok_s.at[0],
                    dst_ref=tok_r.at[turn, :, rows, :],
                    send_sem=tok_send.at[0, 0],
                    recv_sem=tok_recv.at[turn, source],
                    device_id={"row": source},
                    device_id_type=MESH,
                ).wait_recv()

        span = pl.ds(pl.multiple_of(base * mid, mid), mid)
        terms = []
        for v in range(0, 4, 2):
            both = jnp.concatenate([tok_r[turn, v, span, :], tok_r[turn, v + 1, span, :]], axis=1)
            terms.append(dot(high_ref[:, span], both) + dot(low_ref[:, span], both))
        return terms

    def prepare(at):
        for v, term in enumerate(part(at // 2, upper)):
            found[:, 2 * v * LANES : 2 * (v + 1) * LANES] = term

    relayed = jnp.where(central, INNER, OUTER)

    def spread(at):
        side_copy(at, col, beside, 0).start()
        side_copy(at, col, across, 1).start()

        @pl.when(at >= relayed)
        def _():
            side_copy(at, col, corner, 2).start()

    via = beside + core * (across - beside)
    onward = across + core * (beside - across)

    def relay(at):
        side_copy(at, via, via, 2).wait_recv()
        side_copy(at, via, onward, 2).start()

    def finish(at):
        for v, term in enumerate(part(at // 2, 1 - upper)):
            found[:, 2 * v * LANES : 2 * (v + 1) * LANES] += term

    def produce(at):
        turn = at // 2
        sign = (1 - 2 * upper).astype(jnp.float32)
        lone = jnp.logical_and(lane % QUARTER == 0, at == 0)
        straight = jnp.logical_or(cosine_lane, lone)
        weights = []
        for q in range(4):
            angle = math.pi * q / 4
            weights.append(
                (
                    jnp.where(first, 1.0, sign * math.cos(angle)),
                    jnp.where(first, 0.0, sign * math.sin(angle)),
                )
            )
        tall = TALL

        def rows_of(begin):
            rows = pl.ds(begin, tall)
            lower = pl.ds(begin + size, tall)
            re, im = [], []
            for v in range(4):
                span = slice(v * LANES, (v + 1) * LANES)
                a, b = found[rows, span], found[lower, span]
                c, s = turn_c[v, rows], turn_s[v, rows]
                re.append(c * a - s * b)
                im.append(s * a + c * b)
            pr, pi = re[0] + re[2], im[0] + im[2]
            mr, mi = re[0] - re[2], im[0] - im[2]
            sr, si = re[1] + re[3], im[1] + im[3]
            dr, di = re[1] - re[3], im[1] - im[3]
            fours = [
                (pr + sr, pi + si),
                (mr - di, mi + dr),
                (pr - sr, pi - si),
                (mr + di, mi - dr),
            ]
            results = []
            for (a, b), (c, s) in zip(fours, weights):
                xr = c * a - s * b
                xi = s * a + c * b
                keep = jnp.where(straight, xr, -xi)
                move = jnp.where(lone, 0.0, jnp.where(cosine_lane, xi, xr))
                results.append(keep + pltpu.roll(move, QUARTER, 1))
            return results

        def chunk(step, peak):
            begin = pl.multiple_of(step * tall, tall)
            ones = rows_of(begin)
            twos = rows_of(pl.multiple_of(begin + mid, tall))
            for q in range(4):
                value = jnp.where(first, ones[q], twos[q]) + pltpu.roll(
                    jnp.where(first, twos[q], ones[q]), HALF, 1
                )
                packed[q, pl.ds(begin, tall), :] = value
                peak = jnp.maximum(peak, jnp.abs(value))
            return peak

        peak = jnp.zeros((tall, LANES), jnp.float32)
        peak = lax.fori_loop(0, mid // tall, chunk, peak, unroll=UNROLL)
        peak = jnp.max(peak, axis=0, keepdims=True)
        scale = jnp.broadcast_to(jnp.maximum(peak, 1e-30) * 1.0079, (EXTRA, LANES))
        scale = scale.astype(jnp.bfloat16)
        factor = CODE / scale[0:1].astype(jnp.float32)

        @pl.loop(0, 4)
        def _(turn_at):
            q = lax.rem(turn_at + 2 * upper, 4)
            block = packed[q]
            code = jnp.exp(jnp.abs(block) * factor) - 1.0
            code = jnp.where(block < 0.0, -code, code).astype(jnp.bfloat16)
            mine = upper * 4 + q == me

            @pl.when(mine)
            def _():
                gathered[at, col, :mid] = code
                gathered[at, col, mid:] = scale
                spread(at)

            @pl.when(jnp.logical_not(mine))
            def _():
                code_s[turn, q, :mid] = code
                code_s[turn, q, mid:] = scale
                code_copy(at, q).start()

    def forward(at):
        pltpu.make_async_remote_copy(
            src_ref=code_s.at[0, 0],
            dst_ref=gathered.at[at, col],
            send_sem=code_send.at[0, 0],
            recv_sem=code_recv.at[at],
            device_id={"row": row_of(at, upper)},
            device_id_type=MESH,
        ).wait_recv()
        spread(at)

    def contract(at):
        for origin in (onward, corner):
            side_copy(at, origin, origin, 0).wait_recv()

        @pl.when(at >= relayed)
        def _():
            side_copy(at, via, via, 0).wait_recv()

        tops, bottoms = [], []
        for pair_at in range(2):
            values = []
            for c in (2 * pair_at, 2 * pair_at + 1):
                factor = gathered[at, c, mid:].astype(jnp.float32)[0:1] * (scaling / CODE)
                code = gathered[at, c, :mid].astype(jnp.float32)
                value = jnp.log(1.0 + jnp.abs(code)) * factor
                values.append(jnp.where(code < 0.0, -value, value))
            tops.append(jnp.where(first, values[0], pltpu.roll(values[1], HALF, 1)))
            bottoms.append(jnp.where(first, pltpu.roll(values[0], HALF, 1), values[1]))
        for half, parts in enumerate((tops, bottoms)):
            rows = slice(half * mid, (half + 1) * mid)
            high, low = split(jnp.concatenate(parts, axis=1))
            terms = dot(high, fold_high[at]) + dot(low, fold_high[at])
            total[rows] += terms + dot(high, fold_low[at])

    def owns(at):
        return jnp.logical_and(at < SLOTS, jnp.logical_and(central, core == at % 2))

    load_high.wait()
    load_low.wait()
    load_w.wait()

    @pl.when(owns(0))
    def _():
        prepare(0)

    @pl.loop(0, SLOTS + LATE)
    def _(step):
        @pl.when(owns(step))
        def _():
            finish(step)

        @pl.when(jnp.logical_and(step >= LATER, step < relayed + LATER))
        def _():
            relay(step - LATER)

        @pl.when(jnp.logical_and(step >= 1, step < SLOTS + 1))
        def _():
            @pl.when(jnp.logical_not(owns(step - 1)))
            def _():
                forward(step - 1)

        @pl.when(owns(step))
        def _():
            produce(step)

        @pl.when(step >= LATE)
        def _():
            contract(step - LATE)

        @pl.when(step < groups)
        def _():
            fold(step)

        @pl.when(owns(step + 1))
        def _():
            prepare(step + 1)

    out_ref[...] = total[...].astype(jnp.bfloat16)

    @pl.loop(0, SLOTS)
    def _(at):
        near = row_of(at, upper)
        token_copy(at, 1, row_of(at, 1 - upper)).wait_send()

        @pl.when(near != me)
        def _():
            token_copy(at, 0, near).wait_send()

        for which, target in enumerate((beside, across, corner)):
            side_copy(at, col, target, which).wait_send()

        @pl.when(owns(at))
        def _():
            @pl.loop(0, 4)
            def _(q):
                @pl.when(upper * 4 + q != me)
                def _():
                    code_copy(at, q).wait_send()


def kernel_body(tokens, out_weight):
    size = tokens.shape[0]
    length = size * ROWS
    scaling = 1.0 / math.sqrt(length * GROUP_DIM)
    vmem = pl.BlockSpec(memory_space=pltpu.VMEM)
    consts = [jnp.asarray(table) for table in tables(size, length)]
    bf16, f32 = jnp.bfloat16, jnp.float32
    dma = pltpu.SemaphoreType.DMA
    return pl.pallas_call(
        functools.partial(kernel, scaling),
        out_shape=pltpu.VMEM((size, out_weight.shape[1]), bf16),
        in_specs=[pl.BlockSpec(memory_space=pl.ANY)] * 5,
        out_specs=vmem,
        scratch_shapes=[
            pltpu.VMEM((size, size), bf16),
            pltpu.VMEM(out_weight.shape, bf16),
            pltpu.VMEM((2 * size, size), bf16),
            pltpu.VMEM((2 * size, size), bf16),
            pltpu.VMEM((size, LANES), f32),
            pltpu.VMEM((SLOTS, 4, size // RADIX, LANES), bf16),
            pltpu.VMEM((4, 4, size, LANES), bf16),
            pltpu.VMEM((4, size, LANES), f32),
            pltpu.VMEM((4, size, LANES), f32),
            pltpu.VMEM((2 * size, 4 * LANES), f32),
            pltpu.VMEM((4, size // 2, LANES), f32),
            pltpu.VMEM((4, 4, size // 2 + EXTRA, LANES), bf16),
            pltpu.VMEM((SLOTS, COLS, size // 2 + EXTRA, LANES), bf16),
            pltpu.VMEM((SLOTS, COLS * HALF, out_weight.shape[1]), bf16),
            pltpu.VMEM((SLOTS, COLS * HALF, out_weight.shape[1]), bf16),
            pltpu.VMEM((size, out_weight.shape[1]), f32),
            dma((5,)),
            dma((SLOTS, 2)),
            dma((4, ROWS)),
            dma((4, 4)),
            dma((SLOTS,)),
            dma((SLOTS, 3)),
            dma((SLOTS, COLS)),
        ],
        compiler_params=pltpu.CompilerParams(
            collective_id=0, has_side_effects=True, vmem_limit_bytes=60 * 1024 * 1024
        ),
    )(tokens, out_weight, *consts)


def body(tokens, out_weight):
    size = tokens.shape[0]
    fits = (
        lax.axis_size("row") == ROWS
        and lax.axis_size("col") == COLS
        and size == GROUP_DIM
        and tokens.shape[1] == COLS * GROUP_DIM
        and out_weight.shape[1] == GROUP_DIM
    )
    if fits:
        return kernel_body(tokens, out_weight)
    return general_body(tokens, out_weight)


def solution(mesh):
    placed = (P("row", None), P(None, "col"))
    return jax.shard_map(
        body, mesh=mesh, in_specs=placed, out_specs=P("row", "col"), check_vma=False
    )
```

```python
import math

import functools

import jax
import jax.numpy as jnp
import numpy as np
from jax import lax
from jax.experimental import pallas as pl
from jax.experimental.pallas import tpu as pltpu
from jax.sharding import PartitionSpec as P

GROUPS = 4
GROUP_DIM = 512


def angles(product, period):
    return (product % period).astype(jnp.float32) * (2.0 * math.pi / period)


def plain_dot(matrix, values):
    return jnp.dot(
        matrix, values, precision=lax.Precision.HIGHEST, preferred_element_type=jnp.float32
    )


def whole_transform(whole_rows, row_count, seg_rows, length):
    few_chans = whole_rows.shape[2]
    lattice = jnp.arange(row_count, dtype=jnp.int32)
    phases = angles(lattice[:, None] * lattice[None, :], row_count)
    cosine_table = jnp.cos(phases)
    sine_table = jnp.sin(phases)
    real_in = whole_rows[0].reshape(row_count, seg_rows * few_chans)
    imag_in = whole_rows[1].reshape(row_count, seg_rows * few_chans)
    first_re = (plain_dot(cosine_table, real_in) + plain_dot(sine_table, imag_in)).reshape(
        row_count, seg_rows, few_chans
    )
    first_im = (plain_dot(cosine_table, imag_in) - plain_dot(sine_table, real_in)).reshape(
        row_count, seg_rows, few_chans
    )
    inner = jnp.arange(seg_rows, dtype=jnp.int32)
    twist = angles(lattice[:, None] * inner[None, :], length)[:, :, None]
    twist_cos = jnp.cos(twist)
    twist_sin = jnp.sin(twist)
    turned_re = twist_cos * first_re + twist_sin * first_im
    turned_im = twist_cos * first_im - twist_sin * first_re
    folded_re = jnp.transpose(turned_re, (1, 0, 2)).reshape(seg_rows, row_count * few_chans)
    folded_im = jnp.transpose(turned_im, (1, 0, 2)).reshape(seg_rows, row_count * few_chans)
    seg_phases = angles(inner[:, None] * inner[None, :], seg_rows)
    real_part = plain_dot(jnp.cos(seg_phases), folded_re) + plain_dot(
        jnp.sin(seg_phases), folded_im
    )
    return real_part.reshape(length, few_chans)


def general_body(tokens, out_weight):
    seg_rows = tokens.shape[0]
    col_width = out_weight.shape[1]
    row_count = lax.axis_size("row")
    length = seg_rows * row_count
    scaling = 1.0 / math.sqrt(length * GROUP_DIM)
    weight_wide = out_weight.astype(jnp.float32)
    lattice = jnp.arange(GROUP_DIM, dtype=jnp.int32)
    phases = angles(lattice[:, None] * lattice[None, :], GROUP_DIM)
    cosine_table = jnp.cos(phases) * scaling
    sine_table = jnp.sin(phases) * scaling
    folded_rows = []
    for group in range(GROUPS):
        group_rows = weight_wide[group * GROUP_DIM : (group + 1) * GROUP_DIM]
        folded_rows.append(
            jnp.concatenate(
                [plain_dot(cosine_table, group_rows), -plain_dot(sine_table, group_rows)], axis=1
            )
        )
    folded_map = jnp.concatenate(folded_rows, axis=0)
    spectrum = plain_dot(tokens.astype(jnp.float32), folded_map)
    stacked = jnp.stack([spectrum[:, :col_width], spectrum[:, col_width:]])
    whole_rows = lax.all_to_all(stacked, "row", split_axis=2, concat_axis=1, tiled=True)
    ordered = whole_transform(whole_rows, row_count, seg_rows, length)
    spectral = lax.all_to_all(
        ordered.astype(jnp.bfloat16), "row", split_axis=0, concat_axis=1, tiled=True
    )
    return spectral

RADIX = 8
HALF = 64
QUARTER = 32
LANES = 128
EXTRA = 16
ROWS = 8
COLS = 4
SLOTS = 8
CODE = 84.0
LATE = 5
LATER = 3
INNER = 7
OUTER = 6
TALL = 32
UNROLL = 4
MESH = pl.DeviceIdType.MESH


def split_table(values):
    big = values.astype(jnp.bfloat16)
    return big, (values - big.astype(np.float64)).astype(jnp.bfloat16)


def tables(size, length):
    index = np.arange(size)
    phase = 2.0 * np.pi * ((index[:, None] * index[None, :]) % size) / size
    high, low = split_table(np.concatenate([np.cos(phase), np.sin(phase)], axis=0))
    turn = 2.0 * np.pi * (index[:, None] * np.arange(RADIX)[None, :]) / length
    twist = np.zeros((size, LANES), np.float32)
    twist[:, :RADIX] = np.cos(turn)
    twist[:, RADIX : 2 * RADIX] = np.sin(turn)
    return high, low, twist


def dot(a, b):
    return jnp.dot(a, b, preferred_element_type=jnp.float32)


def split(values):
    high = values.astype(jnp.bfloat16)
    return high, (values - high.astype(jnp.float32)).astype(jnp.bfloat16)


def row_of(slot, upper):
    return ROWS // 4 + upper * (ROWS // 4) + slot % 2


def kernel(
    scaling,
    tok_hbm,
    w_hbm,
    high_hbm,
    low_hbm,
    twist_hbm,
    out_ref,
    tok_ref,
    w_ref,
    high_ref,
    low_ref,
    twist_ref,
    tok_s,
    tok_r,
    turn_c,
    turn_s,
    found,
    packed,
    code_s,
    gathered,
    fold_high,
    fold_low,
    total,
    load_sem,
    tok_send,
    tok_recv,
    code_send,
    code_recv,
    side_send,
    side_recv,
):
    me = lax.axis_index("row")
    col = lax.axis_index("col")
    size = tok_ref.shape[0]
    inner = size // RADIX
    mid = size // 2
    groups = COLS
    upper = me // (ROWS // 2)
    central = jnp.logical_and(me >= ROWS // 4, me < 3 * ROWS // 4)
    core = me % 2
    beside = col + 1 - 2 * (col % 2)
    across = col + 2 - 4 * (col // 2)
    corner = COLS - 1 - col

    cols = pl.ds(pl.multiple_of(col * size, size), size)
    load_tok = pltpu.make_async_copy(tok_hbm.at[:, cols], tok_ref, load_sem.at[0])
    load_high = pltpu.make_async_copy(high_hbm, high_ref, load_sem.at[1])
    load_low = pltpu.make_async_copy(low_hbm, low_ref, load_sem.at[2])
    load_w = pltpu.make_async_copy(w_hbm, w_ref, load_sem.at[3])
    load_twist = pltpu.make_async_copy(twist_hbm, twist_ref, load_sem.at[4])
    load_tok.start()
    barrier = pltpu.get_barrier_semaphore()
    for ahead in range(1, ROWS):
        pl.semaphore_signal(
            barrier, inc=1, device_id={"row": lax.rem(me + ahead, ROWS)}, device_id_type=MESH
        )
    for other in (beside, across, corner):
        pl.semaphore_signal(barrier, inc=1, device_id={"col": other}, device_id_type=MESH)

    for load in (load_twist, load_high, load_low, load_w):
        load.start()

    lane = lax.broadcasted_iota(jnp.int32, (1, LANES), 1)
    first = lane < HALF
    cosine_lane = (lane % HALF) < QUARTER

    spot = lax.broadcasted_iota(jnp.int32, (1, size), 1)
    which = spot % HALF
    pair = (spot // HALF) * QUARTER + which % QUARTER
    partner = jnp.where(pair == 0, mid, size - pair)
    wanted = jnp.where(which < QUARTER, pair, partner)
    place = lax.broadcasted_iota(jnp.int32, (size, size), 0)
    pick = jnp.where(place == wanted, 1.0, 0.0).astype(jnp.bfloat16)
    down = lax.broadcasted_iota(jnp.int32, (size, 1), 0)
    residue = 2 * ((down % mid) // inner) + down // mid
    source = RADIX * (down % inner) + residue
    along = lax.broadcasted_iota(jnp.int32, (size, size), 1)
    order = jnp.where(along == source, 1.0, 0.0).astype(jnp.bfloat16)
    def token_copy(at, far, target):
        turn = at // 2
        return pltpu.make_async_remote_copy(
            src_ref=tok_s.at[at],
            dst_ref=tok_r.at[turn, :, pl.ds(pl.multiple_of(me * inner, inner), inner), :],
            send_sem=tok_send.at[at, far],
            recv_sem=tok_recv.at[turn, me],
            device_id={"row": target},
            device_id_type=MESH,
        )

    load_tok.wait()
    for tile in range(COLS):
        span = slice(tile * LANES, (tile + 1) * LANES)
        chosen = dot(tok_ref[...], pick[:, span]).astype(jnp.bfloat16)
        ordered = dot(order, chosen)
        even = ordered[:mid]
        odd = ordered[mid:]
        left = jnp.where(first, even, pltpu.roll(odd, HALF, 1)).astype(jnp.bfloat16)
        right = jnp.where(first, pltpu.roll(even, HALF, 1), odd).astype(jnp.bfloat16)
        for v in range(4):
            tok_s[2 * tile, v] = left[v * inner : (v + 1) * inner]
            tok_s[2 * tile + 1, v] = right[v * inner : (v + 1) * inner]
        if tile == 0:
            pl.semaphore_wait(barrier, ROWS - 1 + COLS - 1)

        @pl.loop(2 * tile, 2 * tile + 2)
        def _(at):
            near = row_of(at, upper)

            @pl.when(near != me)
            def _():
                token_copy(at, 0, near).start()

            token_copy(at, 1, row_of(at, 1 - upper)).start()

            @pl.when(near == me)
            def _():
                rows = pl.ds(pl.multiple_of(me * inner, inner), inner)
                for v in range(4):
                    tok_r[at // 2, v, rows, :] = tok_s[at, v]

    load_twist.wait()
    for v in range(4):
        for start in range(0, size, LANES):
            rows = slice(start, start + LANES)
            turn_c[v, rows] = jnp.where(
                first, twist_ref[rows, 2 * v : 2 * v + 1], twist_ref[rows, 2 * v + 1 : 2 * v + 2]
            )
            turn_s[v, rows] = jnp.where(
                first,
                twist_ref[rows, RADIX + 2 * v : RADIX + 2 * v + 1],
                twist_ref[rows, RADIX + 2 * v + 1 : RADIX + 2 * v + 2],
            )

    parity = lax.broadcasted_iota(jnp.int32, (EXTRA, size), 1) % 2
    swing = (1 - 2 * parity).astype(jnp.float32).astype(jnp.bfloat16)

    def fold(g):
        side = w_ref[pl.ds(pl.multiple_of(g * size, size), size), :]
        wave = dot(high_ref[:mid], side) + dot(low_ref[:mid], side)
        sine = dot(high_ref[size : size + mid], side) + dot(low_ref[size : size + mid], side)
        last = dot(swing, side)[0:1]
        begin = pl.multiple_of(g * HALF, HALF)
        for slot in range(SLOTS):
            rows = slice(slot * QUARTER, (slot + 1) * QUARTER)
            high, low = split(wave[rows])
            fold_high[slot, pl.ds(begin, QUARTER), :] = high
            fold_low[slot, pl.ds(begin, QUARTER), :] = low
            block = -sine[rows]
            if slot == 0:
                top = lax.broadcasted_iota(jnp.int32, block.shape, 0) == 0
                block = jnp.where(top, last, block)
            high, low = split(block)
            begin_odd = pl.multiple_of(g * HALF + QUARTER, QUARTER)
            fold_high[slot, pl.ds(begin_odd, QUARTER), :] = high
            fold_low[slot, pl.ds(begin_odd, QUARTER), :] = low

    total[...] = jnp.zeros_like(total)

    def code_copy(at, quarter):
        return pltpu.make_async_remote_copy(
            src_ref=code_s.at[at // 2, quarter],
            dst_ref=gathered.at[at, col],
            send_sem=code_send.at[at // 2, quarter],
            recv_sem=code_recv.at[at],
            device_id={"row": upper * 4 + quarter},
            device_id_type=MESH,
        )

    def side_copy(at, origin, target, which):
        return pltpu.make_async_remote_copy(
            src_ref=gathered.at[at, origin],
            dst_ref=gathered.at[at, origin],
            send_sem=side_send.at[at, which],
            recv_sem=side_recv.at[at, origin],
            device_id={"col": target},
            device_id_type=MESH,
        )

    def part(turn, base):
        @pl.loop(base * 4, base * 4 + 4)
        def _(source):
            @pl.when(source != me)
            def _():
                rows = pl.ds(pl.multiple_of(source * inner, inner), inner)
                pltpu.make_async_remote_copy(
                    src_ref=tok_s.at[0],
                    dst_ref=tok_r.at[turn, :, rows, :],
                    send_sem=tok_send.at[0, 0],
                    recv_sem=tok_recv.at[turn, source],
                    device_id={"row": source},
                    device_id_type=MESH,
                ).wait_recv()

        span = pl.ds(pl.multiple_of(base * mid, mid), mid)
        terms = []
        for v in range(0, 4, 2):
            both = jnp.concatenate([tok_r[turn, v, span, :], tok_r[turn, v + 1, span, :]], axis=1)
            terms.append(dot(high_ref[:, span], both) + dot(low_ref[:, span], both))
        return terms

    def prepare(at):
        for v, term in enumerate(part(at // 2, upper)):
            found[:, 2 * v * LANES : 2 * (v + 1) * LANES] = term

    relayed = jnp.where(central, INNER, OUTER)

    def spread(at):
        side_copy(at, col, beside, 0).start()
        side_copy(at, col, across, 1).start()

        @pl.when(at >= relayed)
        def _():
            side_copy(at, col, corner, 2).start()

    via = beside + core * (across - beside)
    onward = across + core * (beside - across)

    def relay(at):
        side_copy(at, via, via, 2).wait_recv()
        side_copy(at, via, onward, 2).start()

    def finish(at):
        for v, term in enumerate(part(at // 2, 1 - upper)):
            found[:, 2 * v * LANES : 2 * (v + 1) * LANES] += term

    def produce(at):
        turn = at // 2
        sign = (1 - 2 * upper).astype(jnp.float32)
        lone = jnp.logical_and(lane % QUARTER == 0, at == 0)
        straight = jnp.logical_or(cosine_lane, lone)
        weights = []
        for q in range(4):
            angle = math.pi * q / 4
            weights.append(
                (
                    jnp.where(first, 1.0, sign * math.cos(angle)),
                    jnp.where(first, 0.0, sign * math.sin(angle)),
                )
            )
        tall = TALL

        def rows_of(begin):
            rows = pl.ds(begin, tall)
            lower = pl.ds(begin + size, tall)
            re, im = [], []
            for v in range(4):
                span = slice(v * LANES, (v + 1) * LANES)
                a, b = found[rows, span], found[lower, span]
                c, s = turn_c[v, rows], turn_s[v, rows]
                re.append(c * a - s * b)
                im.append(s * a + c * b)
            pr, pi = re[0] + re[2], im[0] + im[2]
            mr, mi = re[0] - re[2], im[0] - im[2]
            sr, si = re[1] + re[3], im[1] + im[3]
            dr, di = re[1] - re[3], im[1] - im[3]
            fours = [
                (pr + sr, pi + si),
                (mr - di, mi + dr),
                (pr - sr, pi - si),
                (mr + di, mi - dr),
            ]
            results = []
            for (a, b), (c, s) in zip(fours, weights):
                xr = c * a - s * b
                xi = s * a + c * b
                keep = jnp.where(straight, xr, -xi)
                move = jnp.where(lone, 0.0, jnp.where(cosine_lane, xi, xr))
                results.append(keep + pltpu.roll(move, QUARTER, 1))
            return results

        def chunk(step, peak):
            begin = pl.multiple_of(step * tall, tall)
            ones = rows_of(begin)
            twos = rows_of(pl.multiple_of(begin + mid, tall))
            for q in range(4):
                value = jnp.where(first, ones[q], twos[q]) + pltpu.roll(
                    jnp.where(first, twos[q], ones[q]), HALF, 1
                )
                packed[q, pl.ds(begin, tall), :] = value
                peak = jnp.maximum(peak, jnp.abs(value))
            return peak

        peak = jnp.zeros((tall, LANES), jnp.float32)
        peak = lax.fori_loop(0, mid // tall, chunk, peak, unroll=UNROLL)
        peak = jnp.max(peak, axis=0, keepdims=True)
        scale = jnp.broadcast_to(jnp.maximum(peak, 1e-30) * 1.0079, (EXTRA, LANES))
        scale = scale.astype(jnp.bfloat16)
        factor = CODE / scale[0:1].astype(jnp.float32)

        @pl.loop(0, 4)
        def _(turn_at):
            q = lax.rem(turn_at + 2 * upper, 4)
            block = packed[q]
            code = jnp.exp(jnp.abs(block) * factor) - 1.0
            code = jnp.where(block < 0.0, -code, code).astype(jnp.bfloat16)
            mine = upper * 4 + q == me

            @pl.when(mine)
            def _():
                gathered[at, col, :mid] = code
                gathered[at, col, mid:] = scale
                spread(at)

            @pl.when(jnp.logical_not(mine))
            def _():
                code_s[turn, q, :mid] = code
                code_s[turn, q, mid:] = scale
                code_copy(at, q).start()

    def forward(at):
        pltpu.make_async_remote_copy(
            src_ref=code_s.at[0, 0],
            dst_ref=gathered.at[at, col],
            send_sem=code_send.at[0, 0],
            recv_sem=code_recv.at[at],
            device_id={"row": row_of(at, upper)},
            device_id_type=MESH,
        ).wait_recv()
        spread(at)

    def contract(at):
        for origin in (onward, corner):
            side_copy(at, origin, origin, 0).wait_recv()

        @pl.when(at >= relayed)
        def _():
            side_copy(at, via, via, 0).wait_recv()

        tops, bottoms = [], []
        for pair_at in range(2):
            values = []
            for c in (2 * pair_at, 2 * pair_at + 1):
                factor = gathered[at, c, mid:].astype(jnp.float32)[0:1] * (scaling / CODE)
                code = gathered[at, c, :mid].astype(jnp.float32)
                value = jnp.log(1.0 + jnp.abs(code)) * factor
                values.append(jnp.where(code < 0.0, -value, value))
            tops.append(jnp.where(first, values[0], pltpu.roll(values[1], HALF, 1)))
            bottoms.append(jnp.where(first, pltpu.roll(values[0], HALF, 1), values[1]))
        for half, parts in enumerate((tops, bottoms)):
            rows = slice(half * mid, (half + 1) * mid)
            high, low = split(jnp.concatenate(parts, axis=1))
            terms = dot(high, fold_high[at]) + dot(low, fold_high[at])
            terms += dot(high, fold_low[at])

            @pl.when(at < SLOTS - 1)
            def _():
                total[rows] += terms

            @pl.when(at == SLOTS - 1)
            def _():
                out_ref[rows] = (total[rows] + terms).astype(jnp.bfloat16)


    def owns(at):
        return jnp.logical_and(at < SLOTS, jnp.logical_and(central, core == at % 2))

    load_high.wait()
    load_low.wait()
    load_w.wait()

    @pl.when(owns(0))
    def _():
        prepare(0)

    @pl.loop(0, SLOTS + LATE)
    def _(step):
        @pl.when(owns(step))
        def _():
            finish(step)

        @pl.when(jnp.logical_and(step >= LATER, step < relayed + LATER))
        def _():
            relay(step - LATER)

        @pl.when(jnp.logical_and(step >= 1, step < SLOTS + 1))
        def _():
            @pl.when(jnp.logical_not(owns(step - 1)))
            def _():
                forward(step - 1)

        @pl.when(owns(step))
        def _():
            produce(step)

        @pl.when(step >= LATE)
        def _():
            contract(step - LATE)

        @pl.when(step < groups)
        def _():
            fold(step)

        @pl.when(owns(step + 1))
        def _():
            prepare(step + 1)

    @pl.loop(0, SLOTS)
    def _(at):
        near = row_of(at, upper)
        token_copy(at, 1, row_of(at, 1 - upper)).wait_send()

        @pl.when(near != me)
        def _():
            token_copy(at, 0, near).wait_send()

        for which, target in enumerate((beside, across, corner)):
            side_copy(at, col, target, which).wait_send()

        @pl.when(owns(at))
        def _():
            @pl.loop(0, 4)
            def _(q):
                @pl.when(upper * 4 + q != me)
                def _():
                    code_copy(at, q).wait_send()


def kernel_body(tokens, out_weight):
    size = tokens.shape[0]
    length = size * ROWS
    scaling = 1.0 / math.sqrt(length * GROUP_DIM)
    vmem = pl.BlockSpec(memory_space=pltpu.VMEM)
    consts = [jnp.asarray(table) for table in tables(size, length)]
    bf16, f32 = jnp.bfloat16, jnp.float32
    dma = pltpu.SemaphoreType.DMA
    return pl.pallas_call(
        functools.partial(kernel, scaling),
        out_shape=pltpu.VMEM((size, out_weight.shape[1]), bf16),
        in_specs=[pl.BlockSpec(memory_space=pl.ANY)] * 5,
        out_specs=vmem,
        scratch_shapes=[
            pltpu.VMEM((size, size), bf16),
            pltpu.VMEM(out_weight.shape, bf16),
            pltpu.VMEM((2 * size, size), bf16),
            pltpu.VMEM((2 * size, size), bf16),
            pltpu.VMEM((size, LANES), f32),
            pltpu.VMEM((SLOTS, 4, size // RADIX, LANES), bf16),
            pltpu.VMEM((4, 4, size, LANES), bf16),
            pltpu.VMEM((4, size, LANES), f32),
            pltpu.VMEM((4, size, LANES), f32),
            pltpu.VMEM((2 * size, 4 * LANES), f32),
            pltpu.VMEM((4, size // 2, LANES), f32),
            pltpu.VMEM((4, 4, size // 2 + EXTRA, LANES), bf16),
            pltpu.VMEM((SLOTS, COLS, size // 2 + EXTRA, LANES), bf16),
            pltpu.VMEM((SLOTS, COLS * HALF, out_weight.shape[1]), bf16),
            pltpu.VMEM((SLOTS, COLS * HALF, out_weight.shape[1]), bf16),
            pltpu.VMEM((size, out_weight.shape[1]), f32),
            dma((5,)),
            dma((SLOTS, 2)),
            dma((4, ROWS)),
            dma((4, 4)),
            dma((SLOTS,)),
            dma((SLOTS, 3)),
            dma((SLOTS, COLS)),
        ],
        compiler_params=pltpu.CompilerParams(
            collective_id=0, has_side_effects=True, vmem_limit_bytes=60 * 1024 * 1024
        ),
    )(tokens, out_weight, *consts)


def body(tokens, out_weight):
    size = tokens.shape[0]
    fits = (
        lax.axis_size("row") == ROWS
        and lax.axis_size("col") == COLS
        and size == GROUP_DIM
        and tokens.shape[1] == COLS * GROUP_DIM
        and out_weight.shape[1] == GROUP_DIM
    )
    if fits:
        return kernel_body(tokens, out_weight)
    return general_body(tokens, out_weight)


def solution(mesh):
    placed = (P("row", None), P(None, "col"))
    return jax.shard_map(
        body, mesh=mesh, in_specs=placed, out_specs=P("row", "col"), check_vma=False
    )
```
